32 devices in a mesh: sp: 16 (over z, y, x), tp: 2 (over core).
Axes of the slice: x: 2, y: 2, z: 4, core: 2. Of those that a mesh axis runs over, the one named last changes fastest.
Arguments:
- tokens: bfloat16 [4096, 3072], P('sp', 'tp'), may hold values from -6 to 6
- norm_gain: float32 [3072], replicated, may hold values from 0.1 to 1.9
- outer_gate_w: bfloat16 [3072, 1536], P('sp', 'tp'), may hold values from -0.109375 to 0.109375
- inner_gate_w: bfloat16 [3072, 1536], P('sp', 'tp'), may hold values from -0.109375 to 0.109375
- signal_w: bfloat16 [3072, 1536], P('sp', 'tp'), may hold values from -0.109375 to 0.109375
- conv_taps: float32 [3, 1536], P(None, 'tp'), may hold values from -3.5 to 3.5
- query_w: bfloat16 [3072, 1536], P('sp', 'tp'), may hold values from -1.5 to 1.5
- key_w: bfloat16 [3072, 512], P('sp', 'tp'), may hold values from -1.5 to 1.5
- value_w: bfloat16 [3072, 512], P('sp', 'tp'), may hold values from -0.109375 to 0.109375
- sink_logits: float32 [24], P('tp'), may hold values from -1 to 5
- out_conv_w: bfloat16 [1536, 3072], P('tp', 'sp'), may hold values from -0.109375 to 0.109375
- out_attn_w: bfloat16 [1536, 3072], P('tp', 'sp'), may hold values from -0.109375 to 0.109375
Outputs:
- mixed: bfloat16 [4096, 3072], P(('sp', 'tp'))
The draws below stay inside these ranges and needn't reach their ends.
All inputs are finite; a program needn't handle non-finite values.
Results may differ from the reference program's by a relative error of at most 0.02.
Values may be sent and summed in bfloat16 or wider, within the bound.
A program may use at most 64 MiB of HBM per device.

```python
import jax
import jax.numpy as jnp
from jax import lax

D = 3072
CONV = 1536
QHEADS = 24
KVHEADS = 8
HEAD = 64
TAPS = 3
WINDOW = 128
TOKENS = 4096
N_TP = 2


def draw_query_w(key, part):
    drawn = jax.random.normal(jax.random.fold_in(key, 21), (D, QHEADS * HEAD), jnp.float32) * D ** (-0.5)
    return jnp.clip(drawn, -1.5, 1.5).astype(jnp.bfloat16)


def draw_key_w(key, part):
    drawn = jax.random.normal(jax.random.fold_in(key, 22), (D, KVHEADS * HEAD), jnp.float32) * D ** (-0.5)
    return jnp.clip(drawn, -1.5, 1.5).astype(jnp.bfloat16)


def levels(key, dims, split, smallest, largest):
    def one(dim, parts):
        heights = jax.random.uniform(jax.random.fold_in(jax.random.fold_in(key, 6), dim), (parts,), jnp.float32, smallest / len(split), largest / len(split))
        return jnp.repeat(jnp.exp(heights), dims[dim] // parts).reshape((-1,) + (1,) * (len(dims) - dim - 1))

    level = one(*split[0])
    for cut in split[1:]:
        level = level * one(*cut)
    return level


def noise(key, shape, width, most, split=(), kind=jnp.bfloat16):
    entries = jax.random.normal(key, shape, jnp.float32) * width
    if len(split) > 0:
        entries = levels(key, shape, split, -0.22, 0.18) * entries
    return jnp.clip(entries, min=-most, max=most).astype(kind)


def setup_inputs(seed: int = 0) -> dict:
    key_of = jax.random.split(jax.random.key(seed), 13)
    tokens = noise(key_of[0], (TOKENS, D), 1.0, 6.0, ((0, 16), (1, 2)))
    norm_gain = jnp.clip(1.0 + 0.18 * jax.random.normal(key_of[1], (D,), jnp.float32), 0.1, 1.9)
    outer_gate_w = noise(key_of[2], (D, CONV), D ** -0.5, 0.109375, ((0, 16), (1, 2)))
    inner_gate_w = noise(key_of[3], (D, CONV), D ** -0.5, 0.109375, ((0, 16), (1, 2)))
    signal_w = noise(key_of[4], (D, CONV), D ** -0.5, 0.109375, ((0, 16), (1, 2)))
    conv_taps = noise(key_of[5], (TAPS, CONV), TAPS ** -0.5, 3.5, ((1, 2),), jnp.float32)
    query_w = draw_query_w(jax.random.fold_in(key_of[12], 71), 0)
    key_w = draw_key_w(jax.random.fold_in(key_of[12], 71), 0)
    value_w = noise(key_of[8], (D, KVHEADS * HEAD), D ** -0.5, 0.109375, ((0, 16), (1, 2)))
    sink_logits = jnp.clip(-1.0 + 6.0 * jax.random.uniform(key_of[9], (QHEADS,), jnp.float32) ** levels(key_of[9], (QHEADS,), ((0, 2),), -0.2, 0.2), -1.0, 5.0)
    out_conv_w = noise(key_of[10], (CONV, D), (CONV + QHEADS * HEAD) ** -0.5, 0.109375, ((0, 2), (1, 16)))
    out_attn_w = noise(key_of[11], (QHEADS * HEAD, D), (CONV + QHEADS * HEAD) ** -0.5, 0.109375, ((0, 2), (1, 16)))
    return dict(tokens=tokens, norm_gain=norm_gain, outer_gate_w=outer_gate_w, inner_gate_w=inner_gate_w, signal_w=signal_w, conv_taps=conv_taps, query_w=query_w, key_w=key_w, value_w=value_w, sink_logits=sink_logits, out_conv_w=out_conv_w, out_attn_w=out_attn_w)


def reference(tokens, norm_gain, outer_gate_w, inner_gate_w, signal_w, conv_taps, query_w, key_w, value_w, sink_logits, out_conv_w, out_attn_w):
    f32 = jnp.float32
    bf16 = jnp.bfloat16
    x32 = tokens.astype(f32)
    normed = (x32 * lax.rsqrt(lax.optimization_barrier(jnp.mean(x32 * x32, axis=-1, keepdims=True)) + 1e-06) * norm_gain).astype(bf16)

    def project(weight):
        return jnp.dot(normed, weight, preferred_element_type=f32).astype(bf16)
    outer = project(outer_gate_w)
    inner = project(inner_gate_w)
    signal = project(signal_w)
    queries = project(query_w)
    keys = project(key_w)
    values = project(value_w)
    gated = (inner.astype(f32) * signal.astype(f32)).astype(bf16)
    padded = jnp.concatenate([jnp.zeros((TAPS - 1, CONV), bf16), gated], axis=0).astype(f32)
    conv = sum((conv_taps[k] * padded[k:k + TOKENS] for k in range(TAPS)))
    conv_out = (outer.astype(f32) * conv).astype(bf16)
    group = QHEADS // KVHEADS
    span = min(512, TOKENS)
    slopes = jnp.exp2(-8.0 * jnp.arange(1, QHEADS + 1, dtype=f32) / QHEADS).reshape(KVHEADS, group)
    sinks = sink_logits.reshape(KVHEADS, group)[:, :, None]
    keys_pad = jnp.concatenate([jnp.zeros((WINDOW, KVHEADS * HEAD), bf16), keys], axis=0)
    values_pad = jnp.concatenate([jnp.zeros((WINDOW, KVHEADS * HEAD), bf16), values], axis=0)

    def attend(block):
        start = (block * span).astype(jnp.int32)
        qb = lax.dynamic_slice_in_dim(queries, start, span, 0).reshape(span, KVHEADS, group, HEAD).astype(f32)
        kb = lax.dynamic_slice_in_dim(keys_pad, start, span + WINDOW, 0).reshape(span + WINDOW, KVHEADS, HEAD).astype(f32)
        vb = lax.dynamic_slice_in_dim(values_pad, start, span + WINDOW, 0).reshape(span + WINDOW, KVHEADS, HEAD).astype(f32)
        scores = jnp.einsum('qhgd,shd->hgqs', qb, kb) * HEAD ** (-0.5)
        qpos = start + jnp.arange(span, dtype=jnp.int32)
        kpos = start - WINDOW + jnp.arange(span + WINDOW, dtype=jnp.int32)
        dist = qpos[:, None] - kpos[None, :]
        valid = (dist >= 0) & (dist < WINDOW) & (kpos >= 0)[None, :]
        scores = scores - slopes[:, :, None, None] * dist.astype(f32)
        scores = jnp.where(valid, scores, -1e+30)
        top = jnp.maximum(lax.optimization_barrier(jnp.max(scores, axis=-1)), sinks)
        expo = jnp.exp(scores - top[..., None])
        total = lax.optimization_barrier(jnp.sum(expo, axis=-1)) + jnp.exp(sinks - top)
        probs = (expo / total[..., None]).astype(bf16).astype(f32)
        out = jnp.einsum('hgqs,shd->qhgd', probs, vb)
        return out.reshape(span, QHEADS * HEAD)
    attn_out = lax.map(attend, jnp.arange(TOKENS // span, dtype=jnp.int32)).reshape(TOKENS, QHEADS * HEAD).astype(bf16)
    conv_part = CONV // N_TP
    attn_part = QHEADS * HEAD // N_TP
    total_sum = jnp.zeros((TOKENS, D), f32)
    for index in range(N_TP):
        conv_cols = conv_out[:, index * conv_part:(index + 1) * conv_part]
        attn_cols = attn_out[:, index * attn_part:(index + 1) * attn_part]
        partial_value = jnp.dot(conv_cols, out_conv_w[index * conv_part:(index + 1) * conv_part], preferred_element_type=f32)
        partial_value = partial_value + jnp.dot(attn_cols, out_attn_w[index * attn_part:(index + 1) * attn_part], preferred_element_type=f32)
        total_sum = total_sum + partial_value.astype(bf16).astype(f32)
    return total_sum.astype(bf16)
```

```python
import functools

import jax
import jax.numpy as jnp
from jax import lax
from jax.experimental import pallas as pl
from jax.experimental.pallas import tpu as pltpu
from jax.sharding import PartitionSpec as P

QHEADS = 24
KVHEADS = 8
HEAD = 64
TAPS = 3
WINDOW = 128
PLANE = 4
MESH = pl.DeviceIdType.MESH


def from_behind(value, axis, steps):
    count = lax.axis_size(axis)
    initial, last = (max(0, -steps), min(count, count - steps))
    return lax.ppermute(value, axis, [(source, source + steps) for source in range(initial, last)])


def add_products(pieces, normed):
    return tuple((jnp.dot(normed, piece, preferred_element_type=jnp.float32) for piece in pieces))


def convolve(gated, before, outer, conv_taps):
    extended = jnp.concatenate([before, gated], axis=0).astype(jnp.float32)
    length = gated.shape[0]
    conv = sum((conv_taps[k] * extended[k : k + length] for k in range(conv_taps.shape[0])))
    return (outer.astype(jnp.float32) * conv).astype(jnp.bfloat16)


def attention(queries, keys_ext, values_ext, sink_logits, offset):
    f32 = jnp.float32
    length = queries.shape[0]
    kv_local = keys_ext.shape[1] // HEAD
    group = QHEADS // KVHEADS
    heads_local = kv_local * group
    span = min(512, length)
    first = lax.axis_index("tp") * heads_local + 1
    slopes = jnp.exp2(
        -8.0 * (first + jnp.arange(heads_local, dtype=jnp.int32)).astype(f32) / QHEADS
    ).reshape(kv_local, group)
    sinks = sink_logits.reshape(kv_local, group)[:, :, None]

    def attend(block):
        start = block * span
        qblock = queries.reshape(span, kv_local, group, HEAD)
        kblock = keys_ext.reshape(span + WINDOW, kv_local, HEAD)
        vblock = values_ext.reshape(span + WINDOW, kv_local, HEAD)
        scores = jnp.einsum(
            "qhgd,shd->hgqs", qblock, kblock, preferred_element_type=f32
        ) * HEAD ** (-0.5)
        qpos = offset + start + jnp.arange(span, dtype=jnp.int32)
        kpos = offset + start - WINDOW + jnp.arange(span + WINDOW, dtype=jnp.int32)
        dist = qpos[:, None] - kpos[None, :]
        valid = (dist >= 0) & (dist < WINDOW) & (kpos >= 0)[None, :]
        scores = scores - slopes[:, :, None, None] * dist.astype(f32)
        scores = jnp.where(valid, scores, -1e30)
        top = jnp.maximum(jnp.max(scores, axis=-1), sinks)
        expo = jnp.exp(scores - top[..., None])
        total = jnp.sum(expo, axis=-1) + jnp.exp(sinks - top)
        probs = (expo / total[..., None]).astype(jnp.bfloat16)
        out = jnp.einsum("hgqs,shd->qhgd", probs, vblock, preferred_element_type=f32)
        return out.reshape(span, heads_local * HEAD)

    blocks = lax.map(attend, jnp.arange(length // span, dtype=jnp.int32))
    return blocks.reshape(length, heads_local * HEAD).astype(jnp.bfloat16)


def body(
    tokens,
    norm_gain,
    outer_gate_w,
    inner_gate_w,
    signal_w,
    conv_taps,
    query_w,
    key_w,
    value_w,
    sink_logits,
    out_conv_w,
    out_attn_w,
):
    f32 = jnp.float32
    bf16 = jnp.bfloat16
    whole = lax.all_gather(tokens, "tp", axis=1, tiled=True)
    x32 = whole.astype(f32)
    normed = (
        x32 * lax.rsqrt(jnp.mean(x32 * x32, axis=-1, keepdims=True) + 1e-06) * norm_gain
    ).astype(bf16)
    length = normed.shape[0]
    offset = lax.axis_index("sp") * length

    def fold_rows(pieces):
        return add_products(pieces, normed)

    conv_weights = (outer_gate_w, inner_gate_w, signal_w)
    conv_results = fold_rows(
        (
            lax.all_gather(conv_weights[0], "sp", axis=0, tiled=True),
            lax.all_gather(conv_weights[1], "sp", axis=0, tiled=True),
            lax.all_gather(conv_weights[2], "sp", axis=0, tiled=True),
        )
    )
    outer, inner, signal = tuple((result.astype(bf16) for result in conv_results))
    gated = (inner.astype(f32) * signal.astype(f32)).astype(bf16)
    before = from_behind(gated[length - TAPS + 1 :], "sp", 1)
    conv_out = convolve(gated, before, outer, conv_taps)
    attn_weights = (query_w, key_w, value_w)
    attn_results = fold_rows(
        (
            lax.all_gather(attn_weights[0], "sp", axis=0, tiled=True),
            lax.all_gather(attn_weights[1], "sp", axis=0, tiled=True),
            lax.all_gather(attn_weights[2], "sp", axis=0, tiled=True),
        )
    )
    queries, keys, values = tuple((result.astype(bf16) for result in attn_results))
    keys_before, values_before = from_behind(
        (keys[length - WINDOW :], values[length - WINDOW :]), "sp", 1
    )
    keys_ext = jnp.concatenate([keys_before, keys], axis=0)
    values_ext = jnp.concatenate([values_before, values], axis=0)
    attn_out = attention(queries, keys_ext, values_ext, sink_logits, offset)
    conv_whole, attn_whole = (
        lax.all_gather(out_conv_w, "sp", axis=1, tiled=True),
        lax.all_gather(out_attn_w, "sp", axis=1, tiled=True),
    )
    result = jnp.dot(conv_out, conv_whole, preferred_element_type=f32)
    mixed = lax.psum_scatter(
        (result + jnp.dot(attn_out, attn_whole, preferred_element_type=f32)).astype(jnp.bfloat16),
        "tp",
        scatter_dimension=0,
        tiled=True,
    ).astype(jnp.float32)
    return mixed.astype(bf16)


def start_to(src, dst, send_sem, recv_sem, target):
    copy = pltpu.make_async_remote_copy(
        src_ref=src,
        dst_ref=dst,
        send_sem=send_sem,
        recv_sem=recv_sem,
        device_id=target,
        device_id_type=MESH,
    )
    copy.start()
    return copy


def place(count):
    me, core = lax.axis_index("sp"), lax.axis_index("tp")
    return me, core, me // PLANE, lax.rem(me, PLANE), count // PLANE


def greet(me, core, layer, spot, layers):
    barrier = pltpu.get_barrier_semaphore()

    def signal(target):
        pl.semaphore_signal(barrier, inc=1, device_id=target, device_id_type=MESH)

    for k in range(1, PLANE):
        signal({"sp": layer * PLANE + lax.rem(spot + k, PLANE), "tp": core})
    signal({"sp": me, "tp": 1 - core})

    @pl.when(layer + 1 < layers)
    def _():
        signal({"sp": me + PLANE, "tp": core})

    @pl.when(layer > 0)
    def _():
        signal({"sp": me - PLANE, "tp": core})

    beside = jnp.where(layer + 1 < layers, 1, 0) + jnp.where(layer > 0, 1, 0)
    pl.semaphore_wait(barrier, PLANE + beside)


def gather_in_kernel(count, tok_ref, w_ref, x_ref, wg_ref, lsem, ws, wr, ts, tr, ds, dr, us, ur, vs, vr):
    me, core, layer, spot, layers = place(count)
    rows, half = tok_ref.shape
    partner = {"sp": me, "tp": 1 - core}
    above = {"sp": me + PLANE, "tp": core}
    below = {"sp": me - PLANE, "tp": core}
    greet(me, core, layer, spot, layers)

    def peer(k):
        return lax.rem(spot + k, PLANE)

    def source(k):
        return lax.rem(spot + PLANE - k, PLANE)

    def x_slot(p):
        return x_ref.at[pl.ds(pl.multiple_of(p * rows, rows), rows), pl.ds(pl.multiple_of(core * half, half), half)]

    def z_copy(up, d, k, own):
        p = source(k)
        origin = layer - d if up else layer + d
        src = w_ref.at[spot] if own else wg_ref.at[origin, p]
        sems, semr = (us, ur) if up else (vs, vr)
        return pltpu.make_async_remote_copy(
            src_ref=src,
            dst_ref=wg_ref.at[origin, p],
            send_sem=sems.at[d, k],
            recv_sem=semr.at[d, k],
            device_id=above if up else below,
            device_id_type=MESH,
        )

    def z_arrive(up, d, k):
        p = source(k)
        origin = layer - d if up else layer + d
        sems, semr = (us, ur) if up else (vs, vr)
        pltpu.make_async_remote_copy(
            src_ref=w_ref.at[spot],
            dst_ref=wg_ref.at[origin, p],
            send_sem=sems.at[d - 1, k],
            recv_sem=semr.at[d - 1, k],
            device_id=above if up else below,
            device_id_type=MESH,
        ).wait_recv()

    def both(d, k, own, action):
        if d < layers - 1:
            @pl.when((layer + 1 < layers) & (layer >= d))
            def _():
                getattr(z_copy(True, d, k, own), action)()

            @pl.when((layer > 0) & (layer + d < layers))
            def _():
                getattr(z_copy(False, d, k, own), action)()

    both(0, 0, True, "start")
    w_copies = [
        start_to(w_ref.at[peer(k)], wg_ref.at[layer, spot], ws.at[k], wr.at[k], {"sp": layer * PLANE + peer(k), "tp": core})
        for k in range(1, PLANE)
    ]
    t_copies = [
        start_to(tok_ref, x_slot(spot), ts.at[k], tr.at[k], {"sp": layer * PLANE + peer(k), "tp": core})
        for k in range(1, PLANE)
    ]
    d_copies = [start_to(tok_ref, x_slot(spot), ds.at[0], dr.at[0], partner)]
    local = [
        pltpu.make_async_copy(tok_ref, x_slot(spot), lsem.at[0]),
        pltpu.make_async_copy(w_ref.at[spot], wg_ref.at[layer, spot], lsem.at[1]),
    ]
    for copy in local:
        copy.start()
    for k in range(1, PLANE):
        pltpu.make_async_remote_copy(
            src_ref=w_ref.at[spot], dst_ref=wg_ref.at[layer, source(k)], send_sem=ws.at[k], recv_sem=wr.at[k],
            device_id=partner, device_id_type=MESH,
        ).wait_recv()
        both(0, k, False, "start")

    def receive_layer(d):
        for k in range(PLANE):
            @pl.when(layer >= d)
            def _():
                z_arrive(True, d, k)

            @pl.when((layer >= d) & (layer + 1 < layers))
            def _():
                if d < layers - 1:
                    z_copy(True, d, k, False).start()

            @pl.when(layer + d < layers)
            def _():
                z_arrive(False, d, k)

            @pl.when((layer + d < layers) & (layer > 0))
            def _():
                if d < layers - 1:
                    z_copy(False, d, k, False).start()

    if layers > 1:
        receive_layer(1)
    for k in range(1, PLANE):
        p = source(k)
        pltpu.make_async_remote_copy(
            src_ref=tok_ref, dst_ref=x_slot(p), send_sem=ts.at[k], recv_sem=tr.at[k],
            device_id=partner, device_id_type=MESH,
        ).wait_recv()
        d_copies.append(start_to(x_slot(p), x_slot(p), ds.at[k], dr.at[k], partner))
    for d in range(2, layers):
        receive_layer(d)
    for copy in w_copies + t_copies:
        copy.wait_send()
    for k, copy in enumerate(d_copies):
        copy.wait_send()
        p = source(k)
        pltpu.make_async_remote_copy(
            src_ref=tok_ref,
            dst_ref=x_ref.at[pl.ds(pl.multiple_of(p * rows, rows), rows), pl.ds(pl.multiple_of((1 - core) * half, half), half)],
            send_sem=ds.at[k], recv_sem=dr.at[k], device_id=partner, device_id_type=MESH,
        ).wait_recv()
    for d in range(layers - 1):
        for k in range(PLANE):
            both(d, k, d == 0 and k == 0, "wait_send")
    for copy in local:
        copy.wait()


def gather_in(count, tokens, wblocks):
    layers = count // PLANE
    rows, half = tokens.shape
    _, depth, cols = wblocks.shape
    dma = pltpu.SemaphoreType.DMA
    hops = max(layers - 1, 1)
    return pl.pallas_call(
        functools.partial(gather_in_kernel, count),
        out_shape=(
            jax.ShapeDtypeStruct((PLANE * rows, 2 * half), tokens.dtype),
            jax.ShapeDtypeStruct((layers, PLANE, depth, cols), wblocks.dtype),
        ),
        in_specs=[pl.BlockSpec(memory_space=pltpu.VMEM)] * 2,
        out_specs=[pl.BlockSpec(memory_space=pl.ANY)] * 2,
        scratch_shapes=[dma((2,))] + [dma((PLANE,))] * 6 + [dma((hops, PLANE))] * 4,
        compiler_params=pltpu.CompilerParams(collective_id=0, has_side_effects=True),
    )(tokens, wblocks)


def gather_out_kernel(count, h_ref, o_ref, hg_ref, og_ref, held, lsem, ts, tr, ds, dr, us, ur, vs, vr, es, er, fs):
    me, core, layer, spot, layers = place(count)
    width = h_ref.shape[1]
    cols, depth = o_ref.shape
    half = cols // 2
    partner = {"sp": me, "tp": 1 - core}
    above = {"sp": me + PLANE, "tp": core}
    below = {"sp": me - PLANE, "tp": core}
    greet(me, core, layer, spot, layers)

    def peer(k):
        return lax.rem(spot + k, PLANE)

    def source(k):
        return lax.rem(spot + PLANE - k, PLANE)

    def h_slot(c, p):
        return hg_ref.at[:, pl.ds(pl.multiple_of((c * PLANE + p) * width, width), width)]

    def z_copy(up, d, sem_d):
        origin = layer - d if up else layer + d
        sems, semr = (us, ur) if up else (vs, vr)
        return pltpu.make_async_remote_copy(
            src_ref=o_ref if d == 0 else held.at[origin],
            dst_ref=held.at[origin],
            send_sem=sems.at[sem_d],
            recv_sem=semr.at[sem_d],
            device_id=above if up else below,
            device_id_type=MESH,
        )

    def og_slot(origin, c):
        return og_ref.at[pl.ds(pl.multiple_of(origin * half, half), half), pl.ds(pl.multiple_of(c * depth, depth), depth)]

    def part(ref, c):
        return ref.at[pl.ds(pl.multiple_of(c * half, half), half)]

    def pieces(ref, origin, slot):
        swap = pltpu.make_async_remote_copy(
            src_ref=part(ref, 1 - core), dst_ref=og_slot(origin, core), send_sem=es.at[slot], recv_sem=er.at[slot],
            device_id=partner, device_id_type=MESH,
        )
        keep = pltpu.make_async_copy(part(ref, core), og_slot(origin, core), fs.at[slot])
        return swap, keep

    def on_block(up, d, action):
        origin = layer - d if up else layer + d
        if d == 0:
            swap, keep = pieces(o_ref, layer, 0)
        else:
            swap, keep = pieces(held.at[origin], origin, d if up else layers - 1 + d)
        if action == "start":
            swap.start()
            keep.start()
        else:
            swap.wait_send()
            keep.wait()
            pltpu.make_async_remote_copy(
                src_ref=part(o_ref, core), dst_ref=og_slot(origin, 1 - core), send_sem=es.at[0],
                recv_sem=er.at[0 if d == 0 else (d if up else layers - 1 + d)],
                device_id=partner, device_id_type=MESH,
            ).wait_recv()

    def send(d, action):
        if d < layers - 1:
            @pl.when((layer + 1 < layers) & (layer >= d))
            def _():
                getattr(z_copy(True, d, d), action)()

            @pl.when((layer > 0) & (layer + d < layers))
            def _():
                getattr(z_copy(False, d, d), action)()

    send(0, "start")
    t_copies = [
        start_to(h_ref, h_slot(core, spot), ts.at[k], tr.at[k], {"sp": layer * PLANE + peer(k), "tp": core})
        for k in range(1, PLANE)
    ]
    d_copies = [start_to(h_ref, h_slot(core, spot), ds.at[0], dr.at[0], partner)]
    local = pltpu.make_async_copy(h_ref, h_slot(core, spot), lsem.at[0])
    local.start()
    on_block(True, 0, "start")

    def receive_layer(d):
        @pl.when(layer >= d)
        def _():
            z_copy(True, d, d - 1).wait_recv()
            on_block(True, d, "start")

        @pl.when(layer + d < layers)
        def _():
            z_copy(False, d, d - 1).wait_recv()
            on_block(False, d, "start")

        send(d, "start")

    for d in range(1, max(layers - 1, 1)):
        receive_layer(d)
    for k in range(1, PLANE):
        p = source(k)
        pltpu.make_async_remote_copy(
            src_ref=h_ref, dst_ref=h_slot(core, p), send_sem=ts.at[k], recv_sem=tr.at[k],
            device_id=partner, device_id_type=MESH,
        ).wait_recv()
        d_copies.append(start_to(h_slot(core, p), h_slot(core, p), ds.at[k], dr.at[k], partner))
    if layers > 1:
        receive_layer(layers - 1)
    for copy in t_copies:
        copy.wait_send()
    for k, copy in enumerate(d_copies):
        copy.wait_send()
        pltpu.make_async_remote_copy(
            src_ref=h_ref, dst_ref=h_slot(1 - core, source(k)), send_sem=ds.at[k], recv_sem=dr.at[k],
            device_id=partner, device_id_type=MESH,
        ).wait_recv()
    on_block(True, 0, "wait")
    for d in range(layers):
        send(d, "wait_send")
    for d in range(1, layers):
        @pl.when(layer >= d)
        def _():
            on_block(True, d, "wait")

        @pl.when(layer + d < layers)
        def _():
            on_block(False, d, "wait")
    local.wait()


def gather_out(count, hidden, out_t):
    layers = count // PLANE
    rows, width = hidden.shape
    cols, depth = out_t.shape
    dma = pltpu.SemaphoreType.DMA
    hops = max(layers - 1, 1)
    return pl.pallas_call(
        functools.partial(gather_out_kernel, count),
        out_shape=(
            jax.ShapeDtypeStruct((rows, 2 * PLANE * width), hidden.dtype),
            jax.ShapeDtypeStruct((layers * cols // 2, 2 * depth), out_t.dtype),
        ),
        in_specs=[pl.BlockSpec(memory_space=pltpu.VMEM)] * 2,
        out_specs=[pl.BlockSpec(memory_space=pl.ANY)] * 2,
        scratch_shapes=[pltpu.VMEM((layers, cols, depth), out_t.dtype), dma((1,))]
        + [dma((PLANE,))] * 4
        + [dma((hops,))] * 4
        + [dma((2 * layers,))] * 3,
        compiler_params=pltpu.CompilerParams(collective_id=1, has_side_effects=True),
    )(hidden, out_t)


def exchange_kernel(y_ref, out_ref, lsem, ss, rs):
    me, core = lax.axis_index("sp"), lax.axis_index("tp")
    spot = lax.rem(me, PLANE)
    first = me - spot
    mine = spot * 2 + core
    group = 2 * PLANE

    def target(k):
        other = lax.rem(mine + k, group)
        return other, {"sp": first + other // 2, "tp": lax.rem(other, 2)}

    barrier = pltpu.get_barrier_semaphore()
    for k in range(1, group):
        pl.semaphore_signal(barrier, inc=1, device_id=target(k)[1], device_id_type=MESH)
    pl.semaphore_wait(barrier, group - 1)
    copies = []
    for k in range(1, group):
        other, device = target(k)
        copies.append(start_to(y_ref.at[other], out_ref.at[mine], ss.at[k], rs.at[k], device))
    local = pltpu.make_async_copy(y_ref.at[mine], out_ref.at[mine], lsem.at[0])
    local.start()
    for k in range(1, group):
        copies[k - 1].wait_send()
        pltpu.make_async_remote_copy(
            src_ref=y_ref.at[mine], dst_ref=out_ref.at[lax.rem(mine + group - k, group)], send_sem=ss.at[k],
            recv_sem=rs.at[k], device_id=target(k)[1], device_id_type=MESH,
        ).wait_recv()
    local.wait()


def exchange(blocks):
    dma = pltpu.SemaphoreType.DMA
    return pl.pallas_call(
        exchange_kernel,
        out_shape=jax.ShapeDtypeStruct(blocks.shape, blocks.dtype),
        in_specs=[pl.BlockSpec(memory_space=pltpu.VMEM)],
        out_specs=pl.BlockSpec(memory_space=pltpu.VMEM),
        scratch_shapes=[dma((1,)), dma((2 * PLANE,)), dma((2 * PLANE,))],
        compiler_params=pltpu.CompilerParams(collective_id=2, has_side_effects=True),
    )(blocks)


def window_attention(queries, keys_ext, values_ext, sinks, slopes, offset):
    f32 = jnp.float32
    length = queries.shape[0]
    group = QHEADS // KVHEADS
    blocks = length // WINDOW
    qb = queries.reshape(blocks, WINDOW, group, HEAD).transpose(0, 2, 1, 3).reshape(blocks, group * WINDOW, HEAD)

    def pairs(ext):
        cut = ext.reshape(blocks + 1, WINDOW, HEAD)
        return jnp.concatenate([cut[:-1], cut[1:]], axis=1)

    kb, vb = pairs(keys_ext), pairs(values_ext)
    scores = jnp.einsum("bqd,bsd->bqs", qb, kb, preferred_element_type=f32) * HEAD ** (-0.5)
    scores = scores.reshape(blocks, group, WINDOW, 2 * WINDOW)
    dist = WINDOW + jnp.arange(WINDOW, dtype=jnp.int32)[:, None] - jnp.arange(2 * WINDOW, dtype=jnp.int32)[None, :]
    kpos = offset - WINDOW + WINDOW * jnp.arange(blocks, dtype=jnp.int32)[:, None] + jnp.arange(2 * WINDOW, dtype=jnp.int32)[None, :]
    valid = ((dist >= 0) & (dist < WINDOW))[None] & (kpos >= 0)[:, None, :]
    scores = scores - slopes[None, :, None, None] * dist.astype(f32)
    scores = jnp.where(valid[:, None], scores, -1e30)
    sink = sinks[None, :, None]
    top = jnp.maximum(jnp.max(scores, axis=-1), sink)
    expo = jnp.exp(scores - top[..., None])
    total = jnp.sum(expo, axis=-1) + jnp.exp(sink - top)
    probs = (expo / total[..., None]).astype(jnp.bfloat16).reshape(blocks, group * WINDOW, 2 * WINDOW)
    out = jnp.einsum("bqs,bsd->bqd", probs, vb, preferred_element_type=f32)
    out = out.reshape(blocks, group, WINDOW, HEAD).transpose(0, 2, 1, 3)
    return out.reshape(length, group * HEAD).astype(jnp.bfloat16)


def plane_body(
    tokens,
    norm_gain,
    outer_gate_w,
    inner_gate_w,
    signal_w,
    conv_taps,
    query_w,
    key_w,
    value_w,
    sink_logits,
    out_conv_w,
    out_attn_w,
):
    f32 = jnp.float32
    bf16 = jnp.bfloat16
    count = lax.axis_size("sp")
    layers = count // PLANE
    me, core = lax.axis_index("sp"), lax.axis_index("tp")
    layer, spot = me // PLANE, lax.rem(me, PLANE)
    depth = outer_gate_w.shape[0]
    chans = outer_gate_w.shape[1] // PLANE
    wide = query_w.shape[1] // PLANE
    group = QHEADS // KVHEADS

    def cut(weight):
        return weight.reshape(depth, PLANE, -1).transpose(1, 0, 2)

    wblocks = jnp.concatenate(
        [cut(w) for w in (outer_gate_w, inner_gate_w, signal_w, query_w, key_w, value_w)], axis=2
    )
    x, weights = gather_in(count, tokens, wblocks)
    x32 = x.astype(f32)
    normed = (
        x32 * lax.rsqrt(jnp.mean(x32 * x32, axis=-1, keepdims=True) + 1e-06) * norm_gain
    ).astype(bf16)
    proj = jnp.dot(normed, weights.reshape(x.shape[1], -1), preferred_element_type=f32).astype(bf16)
    outer, inner, signal = (proj[:, i * chans : (i + 1) * chans] for i in range(3))
    queries = proj[:, 3 * chans : 3 * chans + wide]
    keys = proj[:, 3 * chans + wide : 3 * chans + wide + HEAD]
    values = proj[:, 3 * chans + wide + HEAD :]
    length = proj.shape[0]
    gated = (inner.astype(f32) * signal.astype(f32)).astype(bf16)
    before = from_behind(gated[length - TAPS + 1 :], "sp", PLANE)
    kv_before = from_behind(proj[length - WINDOW :, 3 * chans + wide :], "sp", PLANE)
    taps = lax.dynamic_slice_in_dim(conv_taps, spot * chans, chans, 1)
    conv_out = convolve(gated, before, outer, taps)
    keys_ext = jnp.concatenate([kv_before[:, :HEAD], keys], axis=0)
    values_ext = jnp.concatenate([kv_before[:, HEAD:], values], axis=0)
    head = (core * PLANE + spot) * group + 1 + jnp.arange(group, dtype=jnp.int32)
    slopes = jnp.exp2(-8.0 * head.astype(f32) / QHEADS)
    sinks = lax.dynamic_slice_in_dim(sink_logits, spot * group, group, 0)
    attn_out = window_attention(queries, keys_ext, values_ext, sinks, slopes, layer * length)
    hidden = jnp.concatenate([conv_out, attn_out], axis=1)
    cols = out_conv_w.shape[1]
    out_t = jnp.concatenate(
        [out_conv_w.reshape(PLANE, chans, cols), out_attn_w.reshape(PLANE, wide, cols)], axis=1
    ).reshape(-1, cols).T
    hidden_all, out_all = gather_out(count, hidden, out_t)
    result = lax.dot_general(
        hidden_all, out_all, (((1,), (1,)), ((), ())), preferred_element_type=f32
    ).astype(bf16)
    swapped = exchange(result.reshape(2 * PLANE, length // (2 * PLANE), -1))
    rows = length // (2 * PLANE)
    swapped = swapped.reshape(PLANE, 2, rows, layers, cols // 2).transpose(2, 3, 0, 1, 4)
    return swapped.reshape(rows, -1)


def solution(mesh):
    kv_local = KVHEADS // mesh.shape["tp"]
    fits = mesh.shape["tp"] == 2 and kv_local == PLANE and mesh.shape["sp"] % PLANE == 0
    chosen = plane_body if fits else body
    in_specs = (
        P("sp", "tp"),
        P(),
        P("sp", "tp"),
        P("sp", "tp"),
        P("sp", "tp"),
        P(None, "tp"),
        P("sp", "tp"),
        P("sp", "tp"),
        P("sp", "tp"),
        P("tp"),
        P("tp", "sp"),
        P("tp", "sp"),
    )
    out_specs = P(("sp", "tp"), None)
    return jax.shard_map(chosen, mesh=mesh, in_specs=in_specs, out_specs=out_specs, check_vma=False)
```

```python
import functools

import jax
import jax.numpy as jnp
from jax import lax
from jax.experimental import pallas as pl
from jax.experimental.pallas import tpu as pltpu
from jax.sharding import PartitionSpec as P

QHEADS = 24
KVHEADS = 8
HEAD = 64
TAPS = 3
WINDOW = 128
PLANE = 4
MESH = pl.DeviceIdType.MESH


def from_behind(value, axis, steps):
    count = lax.axis_size(axis)
    initial, last = (max(0, -steps), min(count, count - steps))
    return lax.ppermute(value, axis, [(source, source + steps) for source in range(initial, last)])


def add_products(pieces, normed):
    return tuple((jnp.dot(normed, piece, preferred_element_type=jnp.float32) for piece in pieces))


def convolve(gated, before, outer, conv_taps):
    extended = jnp.concatenate([before, gated], axis=0).astype(jnp.float32)
    length = gated.shape[0]
    conv = sum((conv_taps[k] * extended[k : k + length] for k in range(conv_taps.shape[0])))
    return (outer.astype(jnp.float32) * conv).astype(jnp.bfloat16)


def attention(queries, keys_ext, values_ext, sink_logits, offset):
    f32 = jnp.float32
    length = queries.shape[0]
    kv_local = keys_ext.shape[1] // HEAD
    group = QHEADS // KVHEADS
    heads_local = kv_local * group
    span = min(512, length)
    first = lax.axis_index("tp") * heads_local + 1
    slopes = jnp.exp2(
        -8.0 * (first + jnp.arange(heads_local, dtype=jnp.int32)).astype(f32) / QHEADS
    ).reshape(kv_local, group)
    sinks = sink_logits.reshape(kv_local, group)[:, :, None]

    def attend(block):
        start = block * span
        qblock = queries.reshape(span, kv_local, group, HEAD)
        kblock = keys_ext.reshape(span + WINDOW, kv_local, HEAD)
        vblock = values_ext.reshape(span + WINDOW, kv_local, HEAD)
        scores = jnp.einsum(
            "qhgd,shd->hgqs", qblock, kblock, preferred_element_type=f32
        ) * HEAD ** (-0.5)
        qpos = offset + start + jnp.arange(span, dtype=jnp.int32)
        kpos = offset + start - WINDOW + jnp.arange(span + WINDOW, dtype=jnp.int32)
        dist = qpos[:, None] - kpos[None, :]
        valid = (dist >= 0) & (dist < WINDOW) & (kpos >= 0)[None, :]
        scores = scores - slopes[:, :, None, None] * dist.astype(f32)
        scores = jnp.where(valid, scores, -1e30)
        top = jnp.maximum(jnp.max(scores, axis=-1), sinks)
        expo = jnp.exp(scores - top[..., None])
        total = jnp.sum(expo, axis=-1) + jnp.exp(sinks - top)
        probs = (expo / total[..., None]).astype(jnp.bfloat16)
        out = jnp.einsum("hgqs,shd->qhgd", probs, vblock, preferred_element_type=f32)
        return out.reshape(span, heads_local * HEAD)

    blocks = lax.map(attend, jnp.arange(length // span, dtype=jnp.int32))
    return blocks.reshape(length, heads_local * HEAD).astype(jnp.bfloat16)


def body(
    tokens,
    norm_gain,
    outer_gate_w,
    inner_gate_w,
    signal_w,
    conv_taps,
    query_w,
    key_w,
    value_w,
    sink_logits,
    out_conv_w,
    out_attn_w,
):
    f32 = jnp.float32
    bf16 = jnp.bfloat16
    whole = lax.all_gather(tokens, "tp", axis=1, tiled=True)
    x32 = whole.astype(f32)
    normed = (
        x32 * lax.rsqrt(jnp.mean(x32 * x32, axis=-1, keepdims=True) + 1e-06) * norm_gain
    ).astype(bf16)
    length = normed.shape[0]
    offset = lax.axis_index("sp") * length

    def fold_rows(pieces):
        return add_products(pieces, normed)

    conv_weights = (outer_gate_w, inner_gate_w, signal_w)
    conv_results = fold_rows(
        (
            lax.all_gather(conv_weights[0], "sp", axis=0, tiled=True),
            lax.all_gather(conv_weights[1], "sp", axis=0, tiled=True),
            lax.all_gather(conv_weights[2], "sp", axis=0, tiled=True),
        )
    )
    outer, inner, signal = tuple((result.astype(bf16) for result in conv_results))
    gated = (inner.astype(f32) * signal.astype(f32)).astype(bf16)
    before = from_behind(gated[length - TAPS + 1 :], "sp", 1)
    conv_out = convolve(gated, before, outer, conv_taps)
    attn_weights = (query_w, key_w, value_w)
    attn_results = fold_rows(
        (
            lax.all_gather(attn_weights[0], "sp", axis=0, tiled=True),
            lax.all_gather(attn_weights[1], "sp", axis=0, tiled=True),
            lax.all_gather(attn_weights[2], "sp", axis=0, tiled=True),
        )
    )
    queries, keys, values = tuple((result.astype(bf16) for result in attn_results))
    keys_before, values_before = from_behind(
        (keys[length - WINDOW :], values[length - WINDOW :]), "sp", 1
    )
    keys_ext = jnp.concatenate([keys_before, keys], axis=0)
    values_ext = jnp.concatenate([values_before, values], axis=0)
    attn_out = attention(queries, keys_ext, values_ext, sink_logits, offset)
    conv_whole, attn_whole = (
        lax.all_gather(out_conv_w, "sp", axis=1, tiled=True),
        lax.all_gather(out_attn_w, "sp", axis=1, tiled=True),
    )
    result = jnp.dot(conv_out, conv_whole, preferred_element_type=f32)
    mixed = lax.psum_scatter(
        (result + jnp.dot(attn_out, attn_whole, preferred_element_type=f32)).astype(jnp.bfloat16),
        "tp",
        scatter_dimension=0,
        tiled=True,
    ).astype(jnp.float32)
    return mixed.astype(bf16)


def start_to(src, dst, send_sem, recv_sem, target):
    copy = pltpu.make_async_remote_copy(
        src_ref=src,
        dst_ref=dst,
        send_sem=send_sem,
        recv_sem=recv_sem,
        device_id=target,
        device_id_type=MESH,
    )
    copy.start()
    return copy


def place(count):
    me, core = lax.axis_index("sp"), lax.axis_index("tp")
    return me, core, me // PLANE, lax.rem(me, PLANE), count // PLANE


def greet(me, core, layer, spot, layers):
    barrier = pltpu.get_barrier_semaphore()

    def signal(target):
        pl.semaphore_signal(barrier, inc=1, device_id=target, device_id_type=MESH)

    for k in range(1, PLANE):
        signal({"sp": layer * PLANE + lax.rem(spot + k, PLANE), "tp": core})
    signal({"sp": me, "tp": 1 - core})

    @pl.when(layer + 1 < layers)
    def _():
        signal({"sp": me + PLANE, "tp": core})

    @pl.when(layer > 0)
    def _():
        signal({"sp": me - PLANE, "tp": core})

    beside = jnp.where(layer + 1 < layers, 1, 0) + jnp.where(layer > 0, 1, 0)
    pl.semaphore_wait(barrier, PLANE + beside)


def gather_in_kernel(count, tok_ref, w_ref, x_ref, wg_ref, lsem, ws, wr, ts, tr, ds, dr, us, ur, vs, vr):
    me, core, layer, spot, layers = place(count)
    rows, half = tok_ref.shape
    partner = {"sp": me, "tp": 1 - core}
    above = {"sp": me + PLANE, "tp": core}
    below = {"sp": me - PLANE, "tp": core}
    greet(me, core, layer, spot, layers)

    def peer(k):
        return lax.rem(spot + k, PLANE)

    def source(k):
        return lax.rem(spot + PLANE - k, PLANE)

    def x_slot(p):
        return x_ref.at[pl.ds(pl.multiple_of(p * rows, rows), rows), pl.ds(pl.multiple_of(core * half, half), half)]

    def z_copy(up, d, k, own):
        p = source(k)
        origin = layer - d if up else layer + d
        src = w_ref.at[spot] if own else wg_ref.at[origin, p]
        sems, semr = (us, ur) if up else (vs, vr)
        return pltpu.make_async_remote_copy(
            src_ref=src,
            dst_ref=wg_ref.at[origin, p],
            send_sem=sems.at[d, k],
            recv_sem=semr.at[d, k],
            device_id=above if up else below,
            device_id_type=MESH,
        )

    def z_arrive(up, d, k):
        p = source(k)
        origin = layer - d if up else layer + d
        sems, semr = (us, ur) if up else (vs, vr)
        pltpu.make_async_remote_copy(
            src_ref=w_ref.at[spot],
            dst_ref=wg_ref.at[origin, p],
            send_sem=sems.at[d - 1, k],
            recv_sem=semr.at[d - 1, k],
            device_id=above if up else below,
            device_id_type=MESH,
        ).wait_recv()

    def both(d, k, own, action):
        if d < layers - 1:
            @pl.when((layer + 1 < layers) & (layer >= d))
            def _():
                getattr(z_copy(True, d, k, own), action)()

            @pl.when((layer > 0) & (layer + d < layers))
            def _():
                getattr(z_copy(False, d, k, own), action)()

    both(0, 0, True, "start")
    w_copies = [
        start_to(w_ref.at[peer(k)], wg_ref.at[layer, spot], ws.at[k], wr.at[k], {"sp": layer * PLANE + peer(k), "tp": core})
        for k in range(1, PLANE)
    ]
    t_copies = [
        start_to(tok_ref, x_slot(spot), ts.at[k], tr.at[k], {"sp": layer * PLANE + peer(k), "tp": core})
        for k in range(1, PLANE)
    ]
    d_copies = [start_to(tok_ref, x_slot(spot), ds.at[0], dr.at[0], partner)]
    local = [
        pltpu.make_async_copy(tok_ref, x_slot(spot), lsem.at[0]),
        pltpu.make_async_copy(w_ref.at[spot], wg_ref.at[layer, spot], lsem.at[1]),
    ]
    for copy in local:
        copy.start()
    for k in range(1, PLANE):
        pltpu.make_async_remote_copy(
            src_ref=w_ref.at[spot], dst_ref=wg_ref.at[layer, source(k)], send_sem=ws.at[k], recv_sem=wr.at[k],
            device_id=partner, device_id_type=MESH,
        ).wait_recv()
        both(0, k, False, "start")

    def receive_layer(d):
        for k in range(PLANE):
            @pl.when(layer >= d)
            def _():
                z_arrive(True, d, k)

            @pl.when((layer >= d) & (layer + 1 < layers))
            def _():
                if d < layers - 1:
                    z_copy(True, d, k, False).start()

            @pl.when(layer + d < layers)
            def _():
                z_arrive(False, d, k)

            @pl.when((layer + d < layers) & (layer > 0))
            def _():
                if d < layers - 1:
                    z_copy(False, d, k, False).start()

    if layers > 1:
        receive_layer(1)
    for k in range(1, PLANE):
        p = source(k)
        pltpu.make_async_remote_copy(
            src_ref=tok_ref, dst_ref=x_slot(p), send_sem=ts.at[k], recv_sem=tr.at[k],
            device_id=partner, device_id_type=MESH,
        ).wait_recv()
        d_copies.append(start_to(x_slot(p), x_slot(p), ds.at[k], dr.at[k], partner))
    for d in range(2, layers):
        receive_layer(d)
    for copy in w_copies + t_copies:
        copy.wait_send()
    for k, copy in enumerate(d_copies):
        copy.wait_send()
        p = source(k)
        pltpu.make_async_remote_copy(
            src_ref=tok_ref,
            dst_ref=x_ref.at[pl.ds(pl.multiple_of(p * rows, rows), rows), pl.ds(pl.multiple_of((1 - core) * half, half), half)],
            send_sem=ds.at[k], recv_sem=dr.at[k], device_id=partner, device_id_type=MESH,
        ).wait_recv()
    for d in range(layers - 1):
        for k in range(PLANE):
            both(d, k, d == 0 and k == 0, "wait_send")
    for copy in local:
        copy.wait()


def gather_in(count, tokens, wblocks):
    layers = count // PLANE
    rows, half = tokens.shape
    _, depth, cols = wblocks.shape
    dma = pltpu.SemaphoreType.DMA
    hops = max(layers - 1, 1)
    return pl.pallas_call(
        functools.partial(gather_in_kernel, count),
        out_shape=(
            jax.ShapeDtypeStruct((PLANE * rows, 2 * half), tokens.dtype),
            jax.ShapeDtypeStruct((layers, PLANE, depth, cols), wblocks.dtype),
        ),
        in_specs=[pl.BlockSpec(memory_space=pltpu.VMEM)] * 2,
        out_specs=[pl.BlockSpec(memory_space=pl.ANY)] * 2,
        scratch_shapes=[dma((2,))] + [dma((PLANE,))] * 6 + [dma((hops, PLANE))] * 4,
        compiler_params=pltpu.CompilerParams(collective_id=0, has_side_effects=True),
    )(tokens, wblocks)


def gather_out_kernel(count, h_ref, o_ref, hg_ref, og_ref, held, lsem, ts, tr, ds, dr, us, ur, vs, vr, es, er, fs):
    me, core, layer, spot, layers = place(count)
    width = h_ref.shape[1]
    cols, depth = o_ref.shape
    half = cols // 2
    partner = {"sp": me, "tp": 1 - core}
    above = {"sp": me + PLANE, "tp": core}
    below = {"sp": me - PLANE, "tp": core}
    greet(me, core, layer, spot, layers)

    def peer(k):
        return lax.rem(spot + k, PLANE)

    def source(k):
        return lax.rem(spot + PLANE - k, PLANE)

    def h_slot(c, p):
        return hg_ref.at[:, pl.ds(pl.multiple_of((c * PLANE + p) * width, width), width)]

    def z_copy(up, d, sem_d):
        origin = layer - d if up else layer + d
        sems, semr = (us, ur) if up else (vs, vr)
        return pltpu.make_async_remote_copy(
            src_ref=o_ref if d == 0 else held.at[origin],
            dst_ref=held.at[origin],
            send_sem=sems.at[sem_d],
            recv_sem=semr.at[sem_d],
            device_id=above if up else below,
            device_id_type=MESH,
        )

    def og_slot(origin, c):
        return og_ref.at[pl.ds(pl.multiple_of(origin * half, half), half), pl.ds(pl.multiple_of(c * depth, depth), depth)]

    def part(ref, c):
        return ref.at[pl.ds(pl.multiple_of(c * half, half), half)]

    def pieces(ref, origin, slot):
        swap = pltpu.make_async_remote_copy(
            src_ref=part(ref, 1 - core), dst_ref=og_slot(origin, core), send_sem=es.at[slot], recv_sem=er.at[slot],
            device_id=partner, device_id_type=MESH,
        )
        keep = pltpu.make_async_copy(part(ref, core), og_slot(origin, core), fs.at[slot])
        return swap, keep

    def on_block(up, d, action):
        origin = layer - d if up else layer + d
        if d == 0:
            swap, keep = pieces(o_ref, layer, 0)
        else:
            swap, keep = pieces(held.at[origin], origin, d if up else layers - 1 + d)
        if action == "start":
            swap.start()
            keep.start()
        else:
            swap.wait_send()
            keep.wait()
            pltpu.make_async_remote_copy(
                src_ref=part(o_ref, core), dst_ref=og_slot(origin, 1 - core), send_sem=es.at[0],
                recv_sem=er.at[0 if d == 0 else (d if up else layers - 1 + d)],
                device_id=partner, device_id_type=MESH,
            ).wait_recv()

    def send(d, action):
        if d < layers - 1:
            @pl.when((layer + 1 < layers) & (layer >= d))
            def _():
                getattr(z_copy(True, d, d), action)()

            @pl.when((layer > 0) & (layer + d < layers))
            def _():
                getattr(z_copy(False, d, d), action)()

    send(0, "start")
    t_copies = [
        start_to(h_ref, h_slot(core, spot), ts.at[k], tr.at[k], {"sp": layer * PLANE + peer(k), "tp": core})
        for k in range(1, PLANE)
    ]
    d_copies = [start_to(h_ref, h_slot(core, spot), ds.at[0], dr.at[0], partner)]
    local = pltpu.make_async_copy(h_ref, h_slot(core, spot), lsem.at[0])
    local.start()
    on_block(True, 0, "start")

    def receive_layer(d):
        @pl.when(layer >= d)
        def _():
            z_copy(True, d, d - 1).wait_recv()
            on_block(True, d, "start")

        @pl.when(layer + d < layers)
        def _():
            z_copy(False, d, d - 1).wait_recv()
            on_block(False, d, "start")

        send(d, "start")

    for d in range(1, max(layers - 1, 1)):
        receive_layer(d)
    for k in range(1, PLANE):
        p = source(k)
        pltpu.make_async_remote_copy(
            src_ref=h_ref, dst_ref=h_slot(core, p), send_sem=ts.at[k], recv_sem=tr.at[k],
            device_id=partner, device_id_type=MESH,
        ).wait_recv()
        d_copies.append(start_to(h_slot(core, p), h_slot(core, p), ds.at[k], dr.at[k], partner))
    if layers > 1:
        receive_layer(layers - 1)
    for copy in t_copies:
        copy.wait_send()
    for k, copy in enumerate(d_copies):
        copy.wait_send()
        pltpu.make_async_remote_copy(
            src_ref=h_ref, dst_ref=h_slot(1 - core, source(k)), send_sem=ds.at[k], recv_sem=dr.at[k],
            device_id=partner, device_id_type=MESH,
        ).wait_recv()
    on_block(True, 0, "wait")
    for d in range(layers):
        send(d, "wait_send")
    for d in range(1, layers):
        @pl.when(layer >= d)
        def _():
            on_block(True, d, "wait")

        @pl.when(layer + d < layers)
        def _():
            on_block(False, d, "wait")
    local.wait()


def gather_out(count, hidden, out_t):
    layers = count // PLANE
    rows, width = hidden.shape
    cols, depth = out_t.shape
    dma = pltpu.SemaphoreType.DMA
    hops = max(layers - 1, 1)
    return pl.pallas_call(
        functools.partial(gather_out_kernel, count),
        out_shape=(
            jax.ShapeDtypeStruct((rows, 2 * PLANE * width), hidden.dtype),
            jax.ShapeDtypeStruct((layers * cols // 2, 2 * depth), out_t.dtype),
        ),
        in_specs=[pl.BlockSpec(memory_space=pltpu.VMEM)] * 2,
        out_specs=[pl.BlockSpec(memory_space=pl.ANY)] * 2,
        scratch_shapes=[pltpu.VMEM((layers, cols, depth), out_t.dtype), dma((1,))]
        + [dma((PLANE,))] * 4
        + [dma((hops,))] * 4
        + [dma((2 * layers,))] * 3,
        compiler_params=pltpu.CompilerParams(collective_id=1, has_side_effects=True),
    )(hidden, out_t)


def exchange_kernel(y_ref, out_ref, lsem, ss, rs):
    me, core = lax.axis_index("sp"), lax.axis_index("tp")
    spot = lax.rem(me, PLANE)
    first = me - spot
    mine = spot * 2 + core
    group = 2 * PLANE

    def target(k):
        other = lax.rem(mine + k, group)
        return other, {"sp": first + other // 2, "tp": lax.rem(other, 2)}

    barrier = pltpu.get_barrier_semaphore()
    for k in range(1, group):
        pl.semaphore_signal(barrier, inc=1, device_id=target(k)[1], device_id_type=MESH)
    pl.semaphore_wait(barrier, group - 1)
    copies = []
    for k in range(1, group):
        other, device = target(k)
        copies.append(start_to(y_ref.at[other], out_ref.at[mine], ss.at[k], rs.at[k], device))
    local = pltpu.make_async_copy(y_ref.at[mine], out_ref.at[mine], lsem.at[0])
    local.start()
    for k in range(1, group):
        copies[k - 1].wait_send()
        pltpu.make_async_remote_copy(
            src_ref=y_ref.at[mine], dst_ref=out_ref.at[lax.rem(mine + group - k, group)], send_sem=ss.at[k],
            recv_sem=rs.at[k], device_id=target(k)[1], device_id_type=MESH,
        ).wait_recv()
    local.wait()


def exchange(blocks):
    dma = pltpu.SemaphoreType.DMA
    return pl.pallas_call(
        exchange_kernel,
        out_shape=jax.ShapeDtypeStruct(blocks.shape, blocks.dtype),
        in_specs=[pl.BlockSpec(memory_space=pltpu.VMEM)],
        out_specs=pl.BlockSpec(memory_space=pltpu.VMEM),
        scratch_shapes=[dma((1,)), dma((2 * PLANE,)), dma((2 * PLANE,))],
        compiler_params=pltpu.CompilerParams(collective_id=2, has_side_effects=True),
    )(blocks)


def pack_kernel(*refs):
    *weights, out_ref = refs
    for p in range(PLANE):
        pieces = []
        for ref in weights:
            width = ref.shape[1] // PLANE
            pieces.append(ref[:, p * width : (p + 1) * width])
        out_ref[p] = jnp.concatenate(pieces, axis=1)


def pack(weights):
    depth = weights[0].shape[0]
    cols = sum(w.shape[1] for w in weights) // PLANE
    return pl.pallas_call(
        pack_kernel,
        out_shape=jax.ShapeDtypeStruct((PLANE, depth, cols), weights[0].dtype),
        in_specs=[pl.BlockSpec(memory_space=pltpu.VMEM)] * len(weights),
        out_specs=pl.BlockSpec(memory_space=pltpu.VMEM),
    )(*weights)


def mixer_kernel(chans, wide, slopes_ref, sinks_ref, offset_ref, proj_ref, before_ref, kv_before_ref, taps_ref, out_ref, ext, gext):
    f32, bf16 = jnp.float32, jnp.bfloat16
    length = proj_ref.shape[0]
    group = wide // HEAD
    front = 8
    ext[0:WINDOW] = kv_before_ref[...]
    ext[WINDOW:] = proj_ref[:, 3 * chans + wide :]
    gext[0:front] = jnp.concatenate(
        [jnp.zeros((front - TAPS + 1, chans), f32), before_ref[...].astype(f32)], axis=0
    )
    row = lax.broadcasted_iota(jnp.int32, (WINDOW, 2 * WINDOW), 0)
    col = lax.broadcasted_iota(jnp.int32, (WINDOW, 2 * WINDOW), 1)
    dist = WINDOW + row - col
    near = (dist >= 0) & (dist < WINDOW)
    far = dist.astype(f32)

    def block(i, carry):
        start = pl.multiple_of(i * WINDOW, WINDOW)
        rows = pl.ds(start, WINDOW)
        chunk = proj_ref[rows, :]
        inner = chunk[:, chans : 2 * chans].astype(f32)
        signal = chunk[:, 2 * chans : 3 * chans].astype(f32)
        gext[pl.ds(pl.multiple_of(start + front, 8), WINDOW), :] = (inner * signal).astype(bf16).astype(f32)
        window = gext[pl.ds(start, WINDOW + front), :]
        conv = sum(
            taps_ref[k : k + 1, :] * window[front - TAPS + 1 + k : front - TAPS + 1 + k + WINDOW]
            for k in range(TAPS)
        )
        pieces = [(chunk[:, :chans].astype(f32) * conv).astype(bf16)]
        kv = ext[pl.ds(start, 2 * WINDOW), :]
        keys, values = kv[:, :HEAD], kv[:, HEAD:]
        valid = near & (offset_ref[0] + start - WINDOW + col >= 0)
        for g in range(group):
            first = 3 * chans + g * HEAD
            scores = lax.dot_general(
                chunk[:, first : first + HEAD], keys, (((1,), (1,)), ((), ())), preferred_element_type=f32
            ) * HEAD ** (-0.5)
            scores = jnp.where(valid, scores - slopes_ref[g] * far, -1e30)
            sink = sinks_ref[g]
            top = jnp.maximum(jnp.max(scores, axis=1, keepdims=True), sink)
            expo = jnp.exp(scores - top)
            total = jnp.sum(expo, axis=1, keepdims=True) + jnp.exp(sink - top)
            probs = (expo / total).astype(bf16)
            pieces.append(jnp.dot(probs, values, preferred_element_type=f32).astype(bf16))
        out_ref[rows, :] = jnp.concatenate(pieces, axis=1)
        return carry

    lax.fori_loop(0, length // WINDOW, block, 0)


def mixer(proj, before, kv_before, taps, slopes, sinks, offset, wide):
    length = proj.shape[0]
    chans = taps.shape[1]
    smem = pl.BlockSpec(memory_space=pltpu.SMEM)
    vmem = pl.BlockSpec(memory_space=pltpu.VMEM)
    return pl.pallas_call(
        functools.partial(mixer_kernel, chans, wide),
        out_shape=jax.ShapeDtypeStruct((length, chans + wide), jnp.bfloat16),
        in_specs=[smem] * 3 + [vmem] * 4,
        out_specs=vmem,
        scratch_shapes=[
            pltpu.VMEM((WINDOW + length, 2 * HEAD), jnp.bfloat16),
            pltpu.VMEM((8 + length, chans), jnp.float32),
        ],
    )(slopes, sinks, jnp.reshape(offset, (1,)), proj, before, kv_before, taps)


def plane_body(
    tokens,
    norm_gain,
    outer_gate_w,
    inner_gate_w,
    signal_w,
    conv_taps,
    query_w,
    key_w,
    value_w,
    sink_logits,
    out_conv_w,
    out_attn_w,
):
    f32 = jnp.float32
    bf16 = jnp.bfloat16
    count = lax.axis_size("sp")
    layers = count // PLANE
    me, core = lax.axis_index("sp"), lax.axis_index("tp")
    layer, spot = me // PLANE, lax.rem(me, PLANE)
    chans = outer_gate_w.shape[1] // PLANE
    wide = query_w.shape[1] // PLANE
    group = QHEADS // KVHEADS

    wblocks = pack((outer_gate_w, inner_gate_w, signal_w, query_w, key_w, value_w))
    x, weights = gather_in(count, tokens, wblocks)
    x32 = x.astype(f32)
    normed = (
        x32 * lax.rsqrt(jnp.mean(x32 * x32, axis=-1, keepdims=True) + 1e-06) * norm_gain
    ).astype(bf16)
    proj = jnp.dot(normed, weights.reshape(x.shape[1], -1), preferred_element_type=f32).astype(bf16)
    length = proj.shape[0]
    last = proj[length - TAPS + 1 :, chans : 3 * chans].astype(f32)
    before = from_behind((last[:, :chans] * last[:, chans:]).astype(bf16), "sp", PLANE)
    kv_before = from_behind(proj[length - WINDOW :, 3 * chans + wide :], "sp", PLANE)
    taps = lax.dynamic_slice_in_dim(conv_taps, spot * chans, chans, 1)
    head = (core * PLANE + spot) * group + 1 + jnp.arange(group, dtype=jnp.int32)
    slopes = jnp.exp2(-8.0 * head.astype(f32) / QHEADS)
    sinks = lax.dynamic_slice_in_dim(sink_logits, spot * group, group, 0)
    hidden = mixer(proj, before, kv_before, taps, slopes, sinks, layer * length, wide)
    cols = out_conv_w.shape[1]
    out_t = jnp.concatenate(
        [out_conv_w.reshape(PLANE, chans, cols), out_attn_w.reshape(PLANE, wide, cols)], axis=1
    ).reshape(-1, cols).T
    hidden_all, out_all = gather_out(count, hidden, out_t)
    result = lax.dot_general(
        hidden_all, out_all, (((1,), (1,)), ((), ())), preferred_element_type=f32
    ).astype(bf16)
    swapped = exchange(result.reshape(2 * PLANE, length // (2 * PLANE), -1))
    rows = length // (2 * PLANE)
    swapped = swapped.reshape(PLANE, 2, rows, layers, cols // 2).transpose(2, 3, 0, 1, 4)
    return swapped.reshape(rows, -1)


def solution(mesh):
    kv_local = KVHEADS // mesh.shape["tp"]
    fits = mesh.shape["tp"] == 2 and kv_local == PLANE and mesh.shape["sp"] % PLANE == 0
    chosen = plane_body if fits else body
    in_specs = (
        P("sp", "tp"),
        P(),
        P("sp", "tp"),
        P("sp", "tp"),
        P("sp", "tp"),
        P(None, "tp"),
        P("sp", "tp"),
        P("sp", "tp"),
        P("sp", "tp"),
        P("tp"),
        P("tp", "sp"),
        P("tp", "sp"),
    )
    out_specs = P(("sp", "tp"), None)
    return jax.shard_map(chosen, mesh=mesh, in_specs=in_specs, out_specs=out_specs, check_vma=False)
```

```python
import functools

import jax
import jax.numpy as jnp
from jax import lax
from jax.experimental import pallas as pl
from jax.experimental.pallas import tpu as pltpu
from jax.sharding import PartitionSpec as P

QHEADS = 24
KVHEADS = 8
HEAD = 64
TAPS = 3
WINDOW = 128
PLANE = 4
MESH = pl.DeviceIdType.MESH


def from_behind(value, axis, steps):
    count = lax.axis_size(axis)
    initial, last = (max(0, -steps), min(count, count - steps))
    return lax.ppermute(value, axis, [(source, source + steps) for source in range(initial, last)])


def add_products(pieces, normed):
    return tuple((jnp.dot(normed, piece, preferred_element_type=jnp.float32) for piece in pieces))


def convolve(gated, before, outer, conv_taps):
    extended = jnp.concatenate([before, gated], axis=0).astype(jnp.float32)
    length = gated.shape[0]
    conv = sum((conv_taps[k] * extended[k : k + length] for k in range(conv_taps.shape[0])))
    return (outer.astype(jnp.float32) * conv).astype(jnp.bfloat16)


def attention(queries, keys_ext, values_ext, sink_logits, offset):
    f32 = jnp.float32
    length = queries.shape[0]
    kv_local = keys_ext.shape[1] // HEAD
    group = QHEADS // KVHEADS
    heads_local = kv_local * group
    span = min(512, length)
    first = lax.axis_index("tp") * heads_local + 1
    slopes = jnp.exp2(
        -8.0 * (first + jnp.arange(heads_local, dtype=jnp.int32)).astype(f32) / QHEADS
    ).reshape(kv_local, group)
    sinks = sink_logits.reshape(kv_local, group)[:, :, None]

    def attend(block):
        start = block * span
        qblock = queries.reshape(span, kv_local, group, HEAD)
        kblock = keys_ext.reshape(span + WINDOW, kv_local, HEAD)
        vblock = values_ext.reshape(span + WINDOW, kv_local, HEAD)
        scores = jnp.einsum(
            "qhgd,shd->hgqs", qblock, kblock, preferred_element_type=f32
        ) * HEAD ** (-0.5)
        qpos = offset + start + jnp.arange(span, dtype=jnp.int32)
        kpos = offset + start - WINDOW + jnp.arange(span + WINDOW, dtype=jnp.int32)
        dist = qpos[:, None] - kpos[None, :]
        valid = (dist >= 0) & (dist < WINDOW) & (kpos >= 0)[None, :]
        scores = scores - slopes[:, :, None, None] * dist.astype(f32)
        scores = jnp.where(valid, scores, -1e30)
        top = jnp.maximum(jnp.max(scores, axis=-1), sinks)
        expo = jnp.exp(scores - top[..., None])
        total = jnp.sum(expo, axis=-1) + jnp.exp(sinks - top)
        probs = (expo / total[..., None]).astype(jnp.bfloat16)
        out = jnp.einsum("hgqs,shd->qhgd", probs, vblock, preferred_element_type=f32)
        return out.reshape(span, heads_local * HEAD)

    blocks = lax.map(attend, jnp.arange(length // span, dtype=jnp.int32))
    return blocks.reshape(length, heads_local * HEAD).astype(jnp.bfloat16)


def body(
    tokens,
    norm_gain,
    outer_gate_w,
    inner_gate_w,
    signal_w,
    conv_taps,
    query_w,
    key_w,
    value_w,
    sink_logits,
    out_conv_w,
    out_attn_w,
):
    f32 = jnp.float32
    bf16 = jnp.bfloat16
    whole = lax.all_gather(tokens, "tp", axis=1, tiled=True)
    x32 = whole.astype(f32)
    normed = (
        x32 * lax.rsqrt(jnp.mean(x32 * x32, axis=-1, keepdims=True) + 1e-06) * norm_gain
    ).astype(bf16)
    length = normed.shape[0]
    offset = lax.axis_index("sp") * length

    def fold_rows(pieces):
        return add_products(pieces, normed)

    conv_weights = (outer_gate_w, inner_gate_w, signal_w)
    conv_results = fold_rows(
        (
            lax.all_gather(conv_weights[0], "sp", axis=0, tiled=True),
            lax.all_gather(conv_weights[1], "sp", axis=0, tiled=True),
            lax.all_gather(conv_weights[2], "sp", axis=0, tiled=True),
        )
    )
    outer, inner, signal = tuple((result.astype(bf16) for result in conv_results))
    gated = (inner.astype(f32) * signal.astype(f32)).astype(bf16)
    before = from_behind(gated[length - TAPS + 1 :], "sp", 1)
    conv_out = convolve(gated, before, outer, conv_taps)
    attn_weights = (query_w, key_w, value_w)
    attn_results = fold_rows(
        (
            lax.all_gather(attn_weights[0], "sp", axis=0, tiled=True),
            lax.all_gather(attn_weights[1], "sp", axis=0, tiled=True),
            lax.all_gather(attn_weights[2], "sp", axis=0, tiled=True),
        )
    )
    queries, keys, values = tuple((result.astype(bf16) for result in attn_results))
    keys_before, values_before = from_behind(
        (keys[length - WINDOW :], values[length - WINDOW :]), "sp", 1
    )
    keys_ext = jnp.concatenate([keys_before, keys], axis=0)
    values_ext = jnp.concatenate([values_before, values], axis=0)
    attn_out = attention(queries, keys_ext, values_ext, sink_logits, offset)
    conv_whole, attn_whole = (
        lax.all_gather(out_conv_w, "sp", axis=1, tiled=True),
        lax.all_gather(out_attn_w, "sp", axis=1, tiled=True),
    )
    result = jnp.dot(conv_out, conv_whole, preferred_element_type=f32)
    mixed = lax.psum_scatter(
        (result + jnp.dot(attn_out, attn_whole, preferred_element_type=f32)).astype(jnp.bfloat16),
        "tp",
        scatter_dimension=0,
        tiled=True,
    ).astype(jnp.float32)
    return mixed.astype(bf16)


def start_to(src, dst, send_sem, recv_sem, target):
    copy = pltpu.make_async_remote_copy(
        src_ref=src,
        dst_ref=dst,
        send_sem=send_sem,
        recv_sem=recv_sem,
        device_id=target,
        device_id_type=MESH,
    )
    copy.start()
    return copy


def place(count):
    me, core = lax.axis_index("sp"), lax.axis_index("tp")
    return me, core, me // PLANE, lax.rem(me, PLANE), count // PLANE


def greet(me, core, layer, spot, layers):
    barrier = pltpu.get_barrier_semaphore()

    def signal(target):
        pl.semaphore_signal(barrier, inc=1, device_id=target, device_id_type=MESH)

    for k in range(1, PLANE):
        signal({"sp": layer * PLANE + lax.rem(spot + k, PLANE), "tp": core})
    signal({"sp": me, "tp": 1 - core})

    @pl.when(layer + 1 < layers)
    def _():
        signal({"sp": me + PLANE, "tp": core})

    @pl.when(layer > 0)
    def _():
        signal({"sp": me - PLANE, "tp": core})

    beside = jnp.where(layer + 1 < layers, 1, 0) + jnp.where(layer > 0, 1, 0)
    pl.semaphore_wait(barrier, PLANE + beside)


def gather_in_kernel(count, tok_ref, w_ref, gain_ref, out_ref, x_ref, wg_ref, nrm_ref, acc_ref, ws, wr, ts, tr, ds, dr, us, ur, vs, vr):
    me, core, layer, spot, layers = place(count)
    rows, half = tok_ref.shape
    partner = {"sp": me, "tp": 1 - core}
    above = {"sp": me + PLANE, "tp": core}
    below = {"sp": me - PLANE, "tp": core}
    greet(me, core, layer, spot, layers)

    def peer(k):
        return lax.rem(spot + k, PLANE)

    def source(k):
        return lax.rem(spot + PLANE - k, PLANE)

    def x_slot(p):
        return x_ref.at[core, pl.ds(pl.multiple_of(p * rows, rows), rows)]

    def z_copy(up, d, k, own):
        p = source(k)
        origin = layer - d if up else layer + d
        src = w_ref.at[spot] if own else wg_ref.at[origin, p]
        sems, semr = (us, ur) if up else (vs, vr)
        return pltpu.make_async_remote_copy(
            src_ref=src,
            dst_ref=wg_ref.at[origin, p],
            send_sem=sems.at[d, k],
            recv_sem=semr.at[d, k],
            device_id=above if up else below,
            device_id_type=MESH,
        )

    def z_arrive(up, d, k):
        p = source(k)
        origin = layer - d if up else layer + d
        sems, semr = (us, ur) if up else (vs, vr)
        pltpu.make_async_remote_copy(
            src_ref=w_ref.at[spot],
            dst_ref=wg_ref.at[origin, p],
            send_sem=sems.at[d - 1, k],
            recv_sem=semr.at[d - 1, k],
            device_id=above if up else below,
            device_id_type=MESH,
        ).wait_recv()

    def both(d, k, own, action):
        if d < layers - 1:
            @pl.when((layer + 1 < layers) & (layer >= d))
            def _():
                getattr(z_copy(True, d, k, own), action)()

            @pl.when((layer > 0) & (layer + d < layers))
            def _():
                getattr(z_copy(False, d, k, own), action)()

    both(0, 0, True, "start")
    w_copies = [
        start_to(w_ref.at[peer(k)], wg_ref.at[layer, spot], ws.at[k], wr.at[k], {"sp": layer * PLANE + peer(k), "tp": core})
        for k in range(1, PLANE)
    ]
    t_copies = [
        start_to(tok_ref, x_slot(spot), ts.at[k], tr.at[k], {"sp": layer * PLANE + peer(k), "tp": core})
        for k in range(1, PLANE)
    ]
    d_copies = [start_to(tok_ref, x_slot(spot), ds.at[0], dr.at[0], partner)]
    x_ref[core, pl.ds(pl.multiple_of(spot * rows, rows), rows), :] = tok_ref[...]
    wg_ref[layer, spot] = w_ref[spot]
    for k in range(1, PLANE):
        pltpu.make_async_remote_copy(
            src_ref=w_ref.at[spot], dst_ref=wg_ref.at[layer, source(k)], send_sem=ws.at[k], recv_sem=wr.at[k],
            device_id=partner, device_id_type=MESH,
        ).wait_recv()
        both(0, k, False, "start")

    def receive_layer(d):
        for k in range(PLANE):
            @pl.when(layer >= d)
            def _():
                z_arrive(True, d, k)

            @pl.when((layer >= d) & (layer + 1 < layers))
            def _():
                if d < layers - 1:
                    z_copy(True, d, k, False).start()

            @pl.when(layer + d < layers)
            def _():
                z_arrive(False, d, k)

            @pl.when((layer + d < layers) & (layer > 0))
            def _():
                if d < layers - 1:
                    z_copy(False, d, k, False).start()

    if layers > 1:
        receive_layer(1)
    for k in range(1, PLANE):
        p = source(k)
        pltpu.make_async_remote_copy(
            src_ref=tok_ref, dst_ref=x_slot(p), send_sem=ts.at[k], recv_sem=tr.at[k],
            device_id=partner, device_id_type=MESH,
        ).wait_recv()
        d_copies.append(start_to(x_slot(p), x_slot(p), ds.at[k], dr.at[k], partner))
    for k in range(PLANE):
        pltpu.make_async_remote_copy(
            src_ref=tok_ref,
            dst_ref=x_ref.at[1 - core, pl.ds(pl.multiple_of(source(k) * rows, rows), rows)],
            send_sem=ds.at[k], recv_sem=dr.at[k], device_id=partner, device_id_type=MESH,
        ).wait_recv()
    length = PLANE * rows
    span = 2 * half // layers
    strip, tall = 32, 256

    def normalise(i, carry):
        at = pl.ds(pl.multiple_of(i * strip, strip), strip)
        whole = jnp.concatenate([x_ref[0, at, :], x_ref[1, at, :]], axis=1).astype(jnp.float32)
        mean = jnp.sum(whole * whole, axis=1, keepdims=True) / (2 * half)
        scaled = (whole * lax.rsqrt(mean + 1e-06) * gain_ref[...]).astype(jnp.bfloat16)
        for j in range(layers):
            nrm_ref[j, at, :] = scaled[:, j * span : (j + 1) * span]
        return carry

    lax.fori_loop(0, length // strip, normalise, 0)

    def add_layer(origin, fresh):
        def step(i, carry):
            at = pl.ds(pl.multiple_of(i * tall, tall), tall)
            product = jnp.dot(
                nrm_ref[origin, at, :],
                wg_ref[origin].reshape(span, wg_ref.shape[3]),
                preferred_element_type=jnp.float32,
            )
            acc_ref[at, :] = product if fresh else acc_ref[at, :] + product
            return carry

        lax.fori_loop(0, length // tall, step, 0)

    def add_both(d):
        @pl.when(layer >= d)
        def _():
            add_layer(layer - d, False)

        @pl.when(layer + d < layers)
        def _():
            add_layer(layer + d, False)

    for d in range(2, layers - 1):
        receive_layer(d)
    add_layer(layer, True)
    for d in range(1, layers - 1):
        add_both(d)
    if layers > 2:
        receive_layer(layers - 1)
    if layers > 1:
        add_both(layers - 1)
    out_ref[...] = acc_ref[...].astype(out_ref.dtype)
    for copy in w_copies + t_copies + d_copies:
        copy.wait_send()
    for d in range(layers - 1):
        for k in range(PLANE):
            both(d, k, d == 0 and k == 0, "wait_send")


def gather_in(count, tokens, wblocks, gain):
    layers = count // PLANE
    rows, half = tokens.shape
    _, depth, cols = wblocks.shape
    dma = pltpu.SemaphoreType.DMA
    hops = max(layers - 1, 1)
    return pl.pallas_call(
        functools.partial(gather_in_kernel, count),
        out_shape=jax.ShapeDtypeStruct((PLANE * rows, cols), jnp.bfloat16),
        in_specs=[pl.BlockSpec(memory_space=pltpu.VMEM)] * 3,
        out_specs=pl.BlockSpec(memory_space=pltpu.VMEM),
        scratch_shapes=[
            pltpu.VMEM((2, PLANE * rows, half), tokens.dtype),
            pltpu.VMEM((layers, PLANE, depth, cols), wblocks.dtype),
            pltpu.VMEM((layers, PLANE * rows, 2 * half // layers), jnp.bfloat16),
            pltpu.VMEM((PLANE * rows, cols), jnp.float32),
        ]
        + [dma((PLANE,))] * 6
        + [dma((hops, PLANE))] * 4,
        compiler_params=pltpu.CompilerParams(
            collective_id=0, has_side_effects=True, vmem_limit_bytes=48 << 20
        ),
    )(tokens, wblocks, gain)


def gather_out_kernel(count, h_ref, o_ref, hg_ref, og_ref, held, lsem, ts, tr, ds, dr, us, ur, vs, vr, es, er, fs):
    me, core, layer, spot, layers = place(count)
    width = h_ref.shape[1]
    cols, depth = o_ref.shape
    half = cols // 2
    partner = {"sp": me, "tp": 1 - core}
    above = {"sp": me + PLANE, "tp": core}
    below = {"sp": me - PLANE, "tp": core}
    greet(me, core, layer, spot, layers)

    def peer(k):
        return lax.rem(spot + k, PLANE)

    def source(k):
        return lax.rem(spot + PLANE - k, PLANE)

    def h_slot(c, p):
        return hg_ref.at[:, pl.ds(pl.multiple_of((c * PLANE + p) * width, width), width)]

    def z_copy(up, d, sem_d):
        origin = layer - d if up else layer + d
        sems, semr = (us, ur) if up else (vs, vr)
        return pltpu.make_async_remote_copy(
            src_ref=o_ref if d == 0 else held.at[origin],
            dst_ref=held.at[origin],
            send_sem=sems.at[sem_d],
            recv_sem=semr.at[sem_d],
            device_id=above if up else below,
            device_id_type=MESH,
        )

    def og_slot(origin, c):
        return og_ref.at[pl.ds(pl.multiple_of(origin * half, half), half), pl.ds(pl.multiple_of(c * depth, depth), depth)]

    def part(ref, c):
        return ref.at[pl.ds(pl.multiple_of(c * half, half), half)]

    def pieces(ref, origin, slot):
        swap = pltpu.make_async_remote_copy(
            src_ref=part(ref, 1 - core), dst_ref=og_slot(origin, core), send_sem=es.at[slot], recv_sem=er.at[slot],
            device_id=partner, device_id_type=MESH,
        )
        keep = pltpu.make_async_copy(part(ref, core), og_slot(origin, core), fs.at[slot])
        return swap, keep

    def on_block(up, d, action):
        origin = layer - d if up else layer + d
        if d == 0:
            swap, keep = pieces(o_ref, layer, 0)
        else:
            swap, keep = pieces(held.at[origin], origin, d if up else layers - 1 + d)
        if action == "start":
            swap.start()
            keep.start()
        else:
            swap.wait_send()
            keep.wait()
            pltpu.make_async_remote_copy(
                src_ref=part(o_ref, core), dst_ref=og_slot(origin, 1 - core), send_sem=es.at[0],
                recv_sem=er.at[0 if d == 0 else (d if up else layers - 1 + d)],
                device_id=partner, device_id_type=MESH,
            ).wait_recv()

    def send(d, action):
        if d < layers - 1:
            @pl.when((layer + 1 < layers) & (layer >= d))
            def _():
                getattr(z_copy(True, d, d), action)()

            @pl.when((layer > 0) & (layer + d < layers))
            def _():
                getattr(z_copy(False, d, d), action)()

    send(0, "start")
    t_copies = [
        start_to(h_ref, h_slot(core, spot), ts.at[k], tr.at[k], {"sp": layer * PLANE + peer(k), "tp": core})
        for k in range(1, PLANE)
    ]
    d_copies = [start_to(h_ref, h_slot(core, spot), ds.at[0], dr.at[0], partner)]
    local = pltpu.make_async_copy(h_ref, h_slot(core, spot), lsem.at[0])
    local.start()
    on_block(True, 0, "start")

    def receive_layer(d):
        @pl.when(layer >= d)
        def _():
            z_copy(True, d, d - 1).wait_recv()
            on_block(True, d, "start")

        @pl.when(layer + d < layers)
        def _():
            z_copy(False, d, d - 1).wait_recv()
            on_block(False, d, "start")

        send(d, "start")

    for d in range(1, max(layers - 1, 1)):
        receive_layer(d)
    for k in range(1, PLANE):
        p = source(k)
        pltpu.make_async_remote_copy(
            src_ref=h_ref, dst_ref=h_slot(core, p), send_sem=ts.at[k], recv_sem=tr.at[k],
            device_id=partner, device_id_type=MESH,
        ).wait_recv()
        d_copies.append(start_to(h_slot(core, p), h_slot(core, p), ds.at[k], dr.at[k], partner))
    if layers > 1:
        receive_layer(layers - 1)
    for copy in t_copies:
        copy.wait_send()
    for k, copy in enumerate(d_copies):
        copy.wait_send()
        pltpu.make_async_remote_copy(
            src_ref=h_ref, dst_ref=h_slot(1 - core, source(k)), send_sem=ds.at[k], recv_sem=dr.at[k],
            device_id=partner, device_id_type=MESH,
        ).wait_recv()
    on_block(True, 0, "wait")
    for d in range(layers):
        send(d, "wait_send")
    for d in range(1, layers):
        @pl.when(layer >= d)
        def _():
            on_block(True, d, "wait")

        @pl.when(layer + d < layers)
        def _():
            on_block(False, d, "wait")
    local.wait()


def gather_out(count, hidden, out_t):
    layers = count // PLANE
    rows, width = hidden.shape
    cols, depth = out_t.shape
    dma = pltpu.SemaphoreType.DMA
    hops = max(layers - 1, 1)
    return pl.pallas_call(
        functools.partial(gather_out_kernel, count),
        out_shape=(
            jax.ShapeDtypeStruct((rows, 2 * PLANE * width), hidden.dtype),
            jax.ShapeDtypeStruct((layers * cols // 2, 2 * depth), out_t.dtype),
        ),
        in_specs=[pl.BlockSpec(memory_space=pltpu.VMEM)] * 2,
        out_specs=[pl.BlockSpec(memory_space=pl.ANY)] * 2,
        scratch_shapes=[pltpu.VMEM((layers, cols, depth), out_t.dtype), dma((1,))]
        + [dma((PLANE,))] * 4
        + [dma((hops,))] * 4
        + [dma((2 * layers,))] * 3,
        compiler_params=pltpu.CompilerParams(collective_id=1, has_side_effects=True),
    )(hidden, out_t)


def exchange_kernel(h_ref, o_ref, out_ref, y_ref, ss, rs):
    me, core = lax.axis_index("sp"), lax.axis_index("tp")
    spot = lax.rem(me, PLANE)
    first = me - spot
    mine = spot * 2 + core
    group = 2 * PLANE

    def target(k):
        other = lax.rem(mine + k, group)
        return other, {"sp": first + other // 2, "tp": lax.rem(other, 2)}

    barrier = pltpu.get_barrier_semaphore()
    for k in range(1, group):
        pl.semaphore_signal(barrier, inc=1, device_id=target(k)[1], device_id_type=MESH)
    pl.semaphore_wait(barrier, group - 1)
    rows = out_ref.shape[1]

    def product(other):
        at = pl.ds(pl.multiple_of(other * rows, rows), rows)
        return lax.dot_general(
            h_ref[at, :], o_ref[...], (((1,), (1,)), ((), ())), preferred_element_type=jnp.float32
        ).astype(out_ref.dtype)

    copies = []

    def send(k):
        copies.append(start_to(y_ref.at[k], out_ref.at[mine], ss.at[k], rs.at[k], target(k)[1]))

    for k in range(1, group):
        y_ref[k] = product(target(k)[0])
        if k > 1:
            send(k - 1)
    out_ref[mine] = product(mine)
    send(group - 1)
    for k in range(1, group):
        copies[k - 1].wait_send()
        pltpu.make_async_remote_copy(
            src_ref=y_ref.at[0], dst_ref=out_ref.at[lax.rem(mine + group - k, group)], send_sem=ss.at[k],
            recv_sem=rs.at[k], device_id=target(k)[1], device_id_type=MESH,
        ).wait_recv()


def exchange(hidden, out_t):
    dma = pltpu.SemaphoreType.DMA
    blocks = (2 * PLANE, hidden.shape[0] // (2 * PLANE), out_t.shape[0])
    return pl.pallas_call(
        exchange_kernel,
        out_shape=jax.ShapeDtypeStruct(blocks, hidden.dtype),
        in_specs=[pl.BlockSpec(memory_space=pltpu.VMEM)] * 2,
        out_specs=pl.BlockSpec(memory_space=pltpu.VMEM),
        scratch_shapes=[pltpu.VMEM(blocks, hidden.dtype), dma((2 * PLANE,)), dma((2 * PLANE,))],
        compiler_params=pltpu.CompilerParams(
            collective_id=2, has_side_effects=True, vmem_limit_bytes=40 << 20
        ),
    )(hidden, out_t)


def pack_kernel(*refs):
    *weights, out_ref = refs
    for p in range(PLANE):
        pieces = []
        for ref in weights:
            width = ref.shape[1] // PLANE
            pieces.append(ref[:, p * width : (p + 1) * width])
        out_ref[p] = jnp.concatenate(pieces, axis=1)


def pack(weights):
    depth = weights[0].shape[0]
    cols = sum(w.shape[1] for w in weights) // PLANE
    return pl.pallas_call(
        pack_kernel,
        out_shape=jax.ShapeDtypeStruct((PLANE, depth, cols), weights[0].dtype),
        in_specs=[pl.BlockSpec(memory_space=pltpu.VMEM)] * len(weights),
        out_specs=pl.BlockSpec(memory_space=pltpu.VMEM),
    )(*weights)


def mixer_kernel(chans, wide, slopes_ref, sinks_ref, offset_ref, proj_ref, before_ref, kv_before_ref, taps_ref, out_ref, ext, gext):
    f32, bf16 = jnp.float32, jnp.bfloat16
    length = proj_ref.shape[0]
    group = wide // HEAD
    front = 8
    ext[0:WINDOW] = kv_before_ref[...]
    ext[WINDOW:] = proj_ref[:, 3 * chans + wide :]
    gext[0:front] = jnp.concatenate(
        [jnp.zeros((front - TAPS + 1, chans), f32), before_ref[...].astype(f32)], axis=0
    )
    row = lax.broadcasted_iota(jnp.int32, (WINDOW, 2 * WINDOW), 0)
    col = lax.broadcasted_iota(jnp.int32, (WINDOW, 2 * WINDOW), 1)
    dist = WINDOW + row - col
    near = (dist >= 0) & (dist < WINDOW)
    far = dist.astype(f32)

    def block(i, carry):
        start = pl.multiple_of(i * WINDOW, WINDOW)
        rows = pl.ds(start, WINDOW)
        chunk = proj_ref[rows, :]
        inner = chunk[:, chans : 2 * chans].astype(f32)
        signal = chunk[:, 2 * chans : 3 * chans].astype(f32)
        gext[pl.ds(pl.multiple_of(start + front, 8), WINDOW), :] = (inner * signal).astype(bf16).astype(f32)
        window = gext[pl.ds(start, WINDOW + front), :]
        conv = sum(
            taps_ref[k : k + 1, :] * window[front - TAPS + 1 + k : front - TAPS + 1 + k + WINDOW]
            for k in range(TAPS)
        )
        pieces = [(chunk[:, :chans].astype(f32) * conv).astype(bf16)]
        kv = ext[pl.ds(start, 2 * WINDOW), :]
        keys, values = kv[:, :HEAD], kv[:, HEAD:]
        valid = near & (offset_ref[0] + start - WINDOW + col >= 0)
        for g in range(group):
            first = 3 * chans + g * HEAD
            scores = lax.dot_general(
                chunk[:, first : first + HEAD], keys, (((1,), (1,)), ((), ())), preferred_element_type=f32
            ) * HEAD ** (-0.5)
            scores = jnp.where(valid, scores - slopes_ref[g] * far, -1e30)
            sink = sinks_ref[g]
            top = jnp.maximum(jnp.max(scores, axis=1, keepdims=True), sink)
            expo = jnp.exp(scores - top)
            total = jnp.sum(expo, axis=1, keepdims=True) + jnp.exp(sink - top)
            probs = (expo / total).astype(bf16)
            pieces.append(jnp.dot(probs, values, preferred_element_type=f32).astype(bf16))
        out_ref[rows, :] = jnp.concatenate(pieces, axis=1)
        return carry

    lax.fori_loop(0, length // WINDOW, block, 0)


def mixer(proj, before, kv_before, taps, slopes, sinks, offset, wide):
    length = proj.shape[0]
    chans = taps.shape[1]
    smem = pl.BlockSpec(memory_space=pltpu.SMEM)
    vmem = pl.BlockSpec(memory_space=pltpu.VMEM)
    return pl.pallas_call(
        functools.partial(mixer_kernel, chans, wide),
        out_shape=jax.ShapeDtypeStruct((length, chans + wide), jnp.bfloat16),
        in_specs=[smem] * 3 + [vmem] * 4,
        out_specs=vmem,
        scratch_shapes=[
            pltpu.VMEM((WINDOW + length, 2 * HEAD), jnp.bfloat16),
            pltpu.VMEM((8 + length, chans), jnp.float32),
        ],
    )(slopes, sinks, jnp.reshape(offset, (1,)), proj, before, kv_before, taps)


def plane_body(
    tokens,
    norm_gain,
    outer_gate_w,
    inner_gate_w,
    signal_w,
    conv_taps,
    query_w,
    key_w,
    value_w,
    sink_logits,
    out_conv_w,
    out_attn_w,
):
    f32 = jnp.float32
    bf16 = jnp.bfloat16
    count = lax.axis_size("sp")
    layers = count // PLANE
    me, core = lax.axis_index("sp"), lax.axis_index("tp")
    layer, spot = me // PLANE, lax.rem(me, PLANE)
    chans = outer_gate_w.shape[1] // PLANE
    wide = query_w.shape[1] // PLANE
    group = QHEADS // KVHEADS

    wblocks = pack((outer_gate_w, inner_gate_w, signal_w, query_w, key_w, value_w))
    proj = gather_in(count, tokens, wblocks, norm_gain.reshape(1, -1))
    length = proj.shape[0]
    last = proj[length - TAPS + 1 :, chans : 3 * chans].astype(f32)
    before = from_behind((last[:, :chans] * last[:, chans:]).astype(bf16), "sp", PLANE)
    kv_before = from_behind(proj[length - WINDOW :, 3 * chans + wide :], "sp", PLANE)
    taps = lax.dynamic_slice_in_dim(conv_taps, spot * chans, chans, 1)
    head = (core * PLANE + spot) * group + 1 + jnp.arange(group, dtype=jnp.int32)
    slopes = jnp.exp2(-8.0 * head.astype(f32) / QHEADS)
    sinks = lax.dynamic_slice_in_dim(sink_logits, spot * group, group, 0)
    hidden = mixer(proj, before, kv_before, taps, slopes, sinks, layer * length, wide)
    cols = out_conv_w.shape[1]
    out_t = jnp.concatenate(
        [out_conv_w.reshape(PLANE, chans, cols), out_attn_w.reshape(PLANE, wide, cols)], axis=1
    ).reshape(-1, cols).T
    hidden_all, out_all = gather_out(count, hidden, out_t)
    swapped = exchange(hidden_all, out_all)
    rows = length // (2 * PLANE)
    swapped = swapped.reshape(PLANE, 2, rows, layers, cols // 2).transpose(2, 3, 0, 1, 4)
    return swapped.reshape(rows, -1)


def solution(mesh):
    kv_local = KVHEADS // mesh.shape["tp"]
    fits = mesh.shape["tp"] == 2 and kv_local == PLANE and mesh.shape["sp"] % PLANE == 0
    chosen = plane_body if fits else body
    in_specs = (
        P("sp", "tp"),
        P(),
        P("sp", "tp"),
        P("sp", "tp"),
        P("sp", "tp"),
        P(None, "tp"),
        P("sp", "tp"),
        P("sp", "tp"),
        P("sp", "tp"),
        P("tp"),
        P("tp", "sp"),
        P("tp", "sp"),
    )
    out_specs = P(("sp", "tp"), None)
    return jax.shard_map(chosen, mesh=mesh, in_specs=in_specs, out_specs=out_specs, check_vma=False)
```
